1024 devices in a mesh: ep: 32 (over z, core), tp: 32 (over y, x).
Axes of the slice: x: 4, y: 8, z: 16, core: 2. Of those that a mesh axis runs over, the one named last changes fastest.
Arguments:
- tokens: bfloat16 [512, 4096], P('ep', 'tp'), may hold values from -40 to 40
- routes: int32 [512, 4], P('ep'), may hold values from 0 to 63, all different within a row; in each aligned block of 16 rows (0 to 15, 16 to 31, ...) at most 2 rows name the same one
- gates: float32 [512, 4], P('ep'), may hold values from 0.1 to 1
- pre_gain: bfloat16 [4096], P('tp'), may hold values from 0.099609375 to 1.8984375
- expert_gate: bfloat16 [64, 4096, 1024], P('ep', 'tp'), may hold values from -0.09375 to 0.09375
- expert_up: bfloat16 [64, 4096, 1024], P('ep', 'tp'), may hold values from -0.09375 to 0.09375
- expert_down: bfloat16 [64, 1024, 4096], P('ep', None, 'tp'), may hold values from -0.125 to 0.125
- shared_gate: bfloat16 [4096, 1024], P('tp'), may hold values from -0.09375 to 0.09375
- shared_up: bfloat16 [4096, 1024], P('tp'), may hold values from -0.09375 to 0.09375
- shared_down: bfloat16 [1024, 4096], P(None, 'tp'), may hold values from -0.125 to 0.125
- out_gain: bfloat16 [4096], P('tp'), may hold values from 0.099609375 to 1.8984375
Outputs:
- mixed: bfloat16 [512, 4096], P('ep', 'tp')
The draws below stay inside these ranges and needn't reach their ends.
Inputs may be any that keep to these rules, and one draw needn't show every extreme that they name: `routes`: each row names 4 different experts, and expert e is held by index e // 2 of ep. Among the 16 rows of one index of ep no expert is named by more than 2 rows, and in every draw some expert is named by exactly 2 rows of some index.
All inputs are finite; a program needn't handle non-finite values.
Results may differ from the reference program's by a relative error of at most 0.012.
Values may be sent and summed in bfloat16 or wider, within the bound.
A program may use at most 32 MiB of HBM per device.

```python
import math
import jax
import jax.numpy as jnp
import numpy as np
from jax import lax

D = 4096
FE = 1024
FS = 1024
TOP = 4
TOK_DEV = 16
EXPERTS = 64
CAP = 2
TOKENS = 512
N_EP = 32


def scaled_columns(key, shape, fan_in):
    first = jax.random.fold_in(key, 0)
    position = jnp.arange(shape[-1], dtype=jnp.float32) / shape[-1]
    base = jnp.clip(jax.random.normal(first, shape, jnp.float32), -4.0, 4.0)
    column = 10.0 ** (position - 1.0)
    return base * column * fan_in ** (-0.5)


def draw_expert_down(key, part):
    return scaled_columns(jax.random.fold_in(key, 11), (EXPERTS, FE, D), FE).astype(jnp.bfloat16)


def draw_shared_down(key, part):
    return scaled_columns(jax.random.fold_in(key, 12), (FS, D), FS).astype(jnp.bfloat16)


def draw_tokens(key, part):
    first, second = jax.random.split(jax.random.fold_in(key, 13), 2)
    position = jnp.arange(D, dtype=jnp.float32) / D
    row_scale = 10.0 ** jax.random.uniform(second, (TOKENS, 1), jnp.float32)
    base = jnp.clip(jax.random.normal(first, (TOKENS, D), jnp.float32), -4.0, 4.0)
    column = 10.0 ** position
    return (base * column * row_scale / 10.0).astype(jnp.bfloat16)


def shard_levels(own_key, shape, cuts, low, high):
    def one(dim, parts):
        heights = jax.random.uniform(jax.random.fold_in(jax.random.fold_in(own_key, 6), dim), (parts,), jnp.float32, low / len(cuts), high / len(cuts))
        return jnp.repeat(jnp.exp(heights), shape[dim] // parts).reshape((-1,) + (1,) * (len(shape) - dim - 1))

    level = one(*cuts[0])
    for cut in cuts[1:]:
        level = level * one(*cut)
    return level


def assign_block(key, own, number, rows, count, top, limit, slope):
    order = jax.random.permutation(key, count)
    crowded, ordinary = load_shares(count, rows * top, limit, slope, True), load_shares(count, rows * top, limit, slope, False)
    places = jnp.arange(count)

    def named(lengths, turn):
        used = int((lengths > 0).sum())
        fixed = max(1, used // 4)
        shifted = fixed + (places - fixed + turn * (used - fixed)) % max(1, count - fixed)
        return jnp.zeros((count,), jnp.int32).at[order[jnp.where(places < fixed, places, shifted)]].set(jnp.asarray(lengths, jnp.int32))

    lengths = jnp.where(number % 4 == 0, named(crowded, number // 4), named(ordinary, number - number // 4 - 1))
    mixed = jax.random.permutation(jax.random.fold_in(own, 3), count)
    giver, taker = mixed[0:count // 2 * 2:2], mixed[1:count // 2 * 2:2]
    margin = jnp.minimum(lengths[giver] - 1, limit - lengths[taker]) // 2
    margin = jnp.where((giver == order[0]) | (taker == order[0]) | (lengths[taker] == 0), 0, jnp.maximum(margin, 0))
    shifted = jax.random.randint(jax.random.fold_in(own, 4), (count // 2,), 0, 1 << 20) % (margin + 1)
    lengths = lengths.at[giver].add(-shifted).at[taker].add(shifted)
    members = jnp.searchsorted(jnp.cumsum(lengths), jnp.arange(rows * top), side="right").astype(jnp.int32)
    table = members.reshape(top, rows).T
    table = table[jax.random.permutation(jax.random.fold_in(own, 1), rows)]
    turn = jax.random.randint(jax.random.fold_in(own, 2), (rows, 1), 0, top)
    return jnp.take_along_axis(table, (jnp.arange(top)[None, :] + turn) % top, axis=1)


def load_shares(number_of, total, most, lean, full):
    loads = [(1 << 20) // math.isqrt(standing ** lean) + 1 for standing in range(1, number_of + 1)]
    largest = most if full else min(most, max(-(-total // number_of), total * loads[0] // sum(loads)))
    least = 1 if total - largest >= number_of - 1 else 0
    given, rest = [largest] + [least] * (number_of - 1), total - largest - least * (number_of - 1)
    while rest > 0:
        movable = [i for i in range(1, number_of) if given[i] < largest] or [i for i in range(1, number_of) if given[i] < most]
        pool, remaining = sum([loads[i] for i in movable]), rest
        for i in movable:
            extra = min(most - given[i], max(1, remaining * loads[i] // pool), rest)
            given[i] = given[i] + extra
            rest = rest - extra
    return np.array(given)


def normal_values(own_key, shape, width, most, pieces=(), held_as=jnp.bfloat16):
    array = jax.random.normal(own_key, shape, jnp.float32) * width
    if len(pieces) > 0:
        array = shard_levels(own_key, shape, pieces, -0.22, 0.18) * array
    return jnp.clip(array, min=-most, max=most).astype(held_as)


def setup_inputs(seed: int = 0) -> dict:
    key_list = jax.random.split(jax.random.key(seed), 12)
    tokens = draw_tokens(jax.random.fold_in(key_list[11], 71), 0)
    routes_keys = jax.random.split(jax.random.fold_in(key_list[1], 1), TOKENS // TOK_DEV)
    routes_turns = jax.random.permutation(jax.random.fold_in(key_list[1], 3), TOKENS // TOK_DEV)
    routes = jax.vmap(lambda own, number: assign_block(jax.random.fold_in(key_list[1], 2), own, number, TOK_DEV, EXPERTS, TOP, CAP, 2))(routes_keys, routes_turns).reshape((TOKENS, TOP))
    gates = jnp.clip(jnp.exp(math.log(1.0) - 2.3025851 * jax.random.uniform(key_list[2], (TOKENS, TOP), jnp.float32) ** shard_levels(key_list[2], (TOKENS, TOP), ((0, 32),), -0.2, 0.2)), 0.1, 1.0)
    pre_gain = jnp.clip(1.0 + 0.18 * jax.random.normal(key_list[3], (D,), jnp.float32), 0.099609375, 1.8984375).astype(jnp.bfloat16)
    expert_gate = normal_values(key_list[4], (EXPERTS, D, FE), D ** -0.5, 0.09375, ((0, 32), (1, 32)))
    expert_up = normal_values(key_list[5], (EXPERTS, D, FE), D ** -0.5, 0.09375, ((0, 32), (1, 32)))
    expert_down = draw_expert_down(jax.random.fold_in(key_list[11], 71), 0)
    shared_gate = normal_values(key_list[7], (D, FS), D ** -0.5, 0.09375, ((0, 32),))
    shared_up = normal_values(key_list[8], (D, FS), D ** -0.5, 0.09375, ((0, 32),))
    shared_down = draw_shared_down(jax.random.fold_in(key_list[11], 71), 0)
    out_gain = jnp.clip(1.0 + 0.18 * jax.random.normal(key_list[10], (D,), jnp.float32), 0.099609375, 1.8984375).astype(jnp.bfloat16)
    return dict(tokens=tokens, routes=routes, gates=gates, pre_gain=pre_gain, expert_gate=expert_gate, expert_up=expert_up, expert_down=expert_down, shared_gate=shared_gate, shared_up=shared_up, shared_down=shared_down, out_gain=out_gain)


def normalize(values, gain):
    as_float = values.astype(jnp.float32)
    scale = lax.rsqrt(lax.optimization_barrier(jnp.mean(as_float * as_float, axis=-1, keepdims=True)) + 1e-06)
    return as_float * scale * gain.astype(jnp.float32)

def reference(tokens, routes, gates, pre_gain, expert_gate, expert_up, expert_down, shared_gate, shared_up, shared_down, out_gain):
    normed = normalize(tokens, pre_gain).astype(jnp.bfloat16)
    labels = jnp.arange(EXPERTS, dtype=jnp.int32)
    picked = routes[:, :, None] == labels[None, None, :]
    onehot = lax.optimization_barrier(jnp.sum(picked.astype(jnp.int32), axis=1))
    dense_gate = lax.optimization_barrier(jnp.sum(jnp.where(picked, gates[:, :, None], jnp.zeros((), jnp.float32)), axis=1))
    blocked = onehot.reshape(N_EP, TOK_DEV, EXPERTS)
    slot_index = (jnp.cumsum(blocked, axis=1) - blocked).reshape(TOKENS, EXPERTS).astype(jnp.int32)
    block_of = jnp.arange(TOKENS, dtype=jnp.int32) // TOK_DEV
    target_row = jnp.where(onehot > 0, block_of[:, None] * CAP + slot_index, -1).astype(jnp.int32)
    row_index = jnp.arange(N_EP * CAP, dtype=jnp.int32)

    def per_expert(accumulated, expert_index):
        select = row_index[:, None] == target_row[:, expert_index][None, :]
        buffer = jnp.dot(select.astype(jnp.bfloat16), normed, preferred_element_type=jnp.float32).astype(jnp.bfloat16)
        gate_act = jnp.dot(buffer, expert_gate[expert_index], preferred_element_type=jnp.float32)
        up_act = jnp.dot(buffer, expert_up[expert_index], preferred_element_type=jnp.float32)
        hidden = (jax.nn.silu(gate_act) * up_act).astype(jnp.bfloat16)
        result = jnp.dot(hidden, expert_down[expert_index], preferred_element_type=jnp.float32).astype(jnp.bfloat16)
        weight = jnp.where(select, dense_gate[:, expert_index][None, :], jnp.zeros((), jnp.float32))
        accumulated = accumulated + jnp.dot(weight.T, result.astype(jnp.float32), precision=lax.Precision.HIGHEST)
        return (accumulated, None)
    routed, _ = lax.scan(per_expert, jnp.zeros((TOKENS, D), jnp.float32), jnp.arange(EXPERTS, dtype=jnp.int32))
    shared_gate_act = jnp.dot(normed, shared_gate, preferred_element_type=jnp.float32)
    shared_up_act = jnp.dot(normed, shared_up, preferred_element_type=jnp.float32)
    shared_hidden = (jax.nn.silu(shared_gate_act) * shared_up_act).astype(jnp.bfloat16)
    shared_out = jnp.dot(shared_hidden, shared_down, preferred_element_type=jnp.float32)
    combined = routed + shared_out
    return normalize(combined, out_gain).astype(jnp.bfloat16)
```

```python
import jax
import jax.numpy as jnp
from jax import lax
from jax.experimental import pallas as pl
from jax.experimental.pallas import tpu as pltpu
from jax.sharding import PartitionSpec as P

MESH = pl.DeviceIdType.MESH
BF = jnp.bfloat16
F32 = jnp.float32
D = 4096.0
EPS = 1e-06
NX, NY, NZ = 4, 8, 16
NEP, NTP = 32, 32
DYS = (4, 3, 5, 2, 6, 1, 7, 0)
NT = (((1,), (1,)), ((), ()))
NN = (((1,), (0,)), ((), ()))


def dot(a, b, dims=NN):
    return lax.dot_general(a, b, dims, preferred_element_type=F32)


def ep_target(i, z, c):
    j = i // 2
    k = (j + 1) // 2
    dz = jnp.where(j % 2 == 0, 8 + k, 8 - k)
    core = (c + 1 + i) % 2
    return ((z + dz) % NZ) * 2 + core


def tp_target(i, y, x):
    j = i // 4
    k = (j + 1) // 2
    dy = jnp.where(j % 2 == 0, 4 + k, 4 - k)
    dx = 2 + i % 4
    dx = jnp.where(i % 4 == 1, 1, jnp.where(i % 4 == 2, 3, jnp.where(i % 4 == 3, 0, 2)))
    return ((y + dy) % NY) * NX + (x + dx) % NX


def kernel(
    tok_h, routes_h, gates_h, pg_h, eg_h, eu_h, ed_h, sg_h, su_h, sd_h, og_h,
    out_ref,
    tok, routes, gates, pg, eg, eu, ed, sg, su, sd, og,
    wt, swt, dt, asend, arecv, rows, tail, xbd, sxbd,
    xsend, xrecv, ysend, yrecv, hid, hsh, dsend, drecv, esend, erecv,
    in_sem, a_s, a_r, bx_s, bx_r, by_s, by_r, c_s, c_r, cs_s, cs_r, d_s, d_r, e_s, e_r,
):
    me_ep, me_tp = lax.axis_index("ep"), lax.axis_index("tp")
    z, c = me_ep // 2, me_ep % 2
    y, x = me_tp // NX, me_tp % NX

    barrier = pltpu.get_barrier_semaphore()

    def greet(i, carry):
        pl.semaphore_signal(barrier, inc=1, device_id=(ep_target(i, z, c), me_tp), device_id_type=MESH)
        pl.semaphore_signal(barrier, inc=1, device_id=(me_ep, tp_target(i, y, x)), device_id_type=MESH)
        return carry

    lax.fori_loop(0, 31, greet, 0)

    pairs = (
        (tok_h, tok), (routes_h, routes), (gates_h, gates), (pg_h, pg), (og_h, og),
        (eg_h, eg), (eu_h, eu), (sg_h, sg), (su_h, su), (ed_h, ed), (sd_h, sd),
    )
    loads = [pltpu.make_async_copy(a, b, in_sem.at[k]) for k, (a, b) in enumerate(pairs)]
    for load in loads:
        load.start()
    for load in loads[:5]:
        load.wait()

    lane = lax.broadcasted_iota(jnp.int32, (16, 128), 1)
    sub = lax.broadcasted_iota(jnp.int32, (16, 128), 0)
    named = jnp.zeros((16, 128), F32)
    weight = jnp.zeros((16, 128), F32)
    for k in range(4):
        hit = routes[:, k : k + 1] == lane // 2
        named = named + jnp.where(hit, 1.0, 0.0)
        weight = weight + jnp.where(hit, gates[:, k : k + 1], 0.0)
    low = jnp.where(
        lax.broadcasted_iota(jnp.int32, (16, 16), 1) < lax.broadcasted_iota(jnp.int32, (16, 16), 0), 1.0, 0.0
    )
    slot = dot(low.astype(BF), named.astype(BF))
    chosen = (named > 0.5) & (jnp.abs(slot - (lane % 2).astype(F32)) < 0.5)
    select = jnp.where(chosen, 1.0, 0.0)
    weight = jnp.where(chosen, weight, 0.0)
    own = tok[...]
    rows[...] = dot(select.T.astype(BF), own)
    for b in range(NEP):
        asend[b] = rows[4 * b : 4 * b + 4, :].astype(BF)

    for load in loads[5:7]:
        load.wait()
    for k in range(8):
        for half, source in enumerate((eg, eu)):
            for e in range(2):
                wt[k, 128 * half : 128 * half + 128, 128 * e : 128 * e + 128] = source[
                    e, :, 128 * k : 128 * k + 128
                ].T

    pl.semaphore_wait(barrier, 62)

    def dispatch(i, carry):
        to = ep_target(i, z, c)
        pltpu.make_async_remote_copy(
            src_ref=asend.at[to], dst_ref=arecv.at[me_ep], send_sem=a_s, recv_sem=a_r,
            device_id=(to, me_tp), device_id_type=MESH,
        ).start()
        return carry

    lax.fori_loop(0, 31, dispatch, 0)
    arecv[me_ep] = asend[me_ep]

    for load in loads[7:]:
        load.wait()
    for k in range(8):
        for half, source in enumerate((sg, su)):
            swt[128 * half : 128 * half + 128, 128 * k : 128 * k + 128] = source[:, 128 * k : 128 * k + 128].T
        for e in range(2):
            dt[128 * e : 128 * e + 128, 128 * k : 128 * k + 128] = ed[e, 128 * k : 128 * k + 128, :].T
    gain = pg[...].astype(F32)
    own32 = own.astype(F32)
    sxbd[...] = jnp.zeros_like(sxbd)
    own_gained = (own32 * gain).astype(BF)
    for g in range(8):
        sxbd[16 * g : 16 * g + 16, 128 * g : 128 * g + 128] = own_gained
    rows2 = dot(swt[...], sxbd[...], NT)
    own_squares = jnp.sum(own32 * own32, axis=1, keepdims=True)
    own_line = jnp.sum(jnp.where(lane % 16 == sub, own_squares, 0.0), axis=0, keepdims=True)
    own_line_hi = own_line.astype(BF).astype(F32)
    tail[...] = jnp.zeros_like(tail)
    for p in range(NTP):
        tail[p, 0:4, :] = rows2[4 * p : 4 * p + 4, :]
        tail[p, 4:8, :] = rows2[128 + 4 * p : 132 + 4 * p, :]

    pltpu.make_async_copy(arecv.at[pl.ds(0, 31)], arecv.at[pl.ds(0, 31)], a_r).wait()
    for b in range(NEP):
        rows[4 * b : 4 * b + 4, :] = arecv[b].astype(F32)
    came = rows[...]
    r0 = lax.broadcasted_iota(jnp.int32, (128, 128), 0)
    r1 = lax.broadcasted_iota(jnp.int32, (128, 128), 1)
    squares = jnp.sum(came * came, axis=1, keepdims=True)
    line = jnp.sum(jnp.where(r0 == r1, squares, 0.0), axis=0, keepdims=True)
    line_hi = line.astype(BF).astype(F32)
    came_gained = came * gain
    first = (r0 // 2) % 2 == 0
    xbd[:, 0:128] = jnp.where(first, came_gained, 0.0).astype(BF)
    xbd[:, 128:256] = jnp.where(first, 0.0, came_gained).astype(BF)
    sums = jnp.where(sub == 8, line_hi, 0.0) + jnp.where(sub == 9, line - line_hi, 0.0)
    sums = sums + jnp.where(sub == 10, own_line_hi, 0.0) + jnp.where(sub == 11, own_line - own_line_hi, 0.0)

    for dy in DYS:
        yp = (y + dy) % NY
        part = dot(wt[yp], xbd[...], NT)
        for xp in range(NX):
            xsend[yp, xp, 0:32, :] = part[32 * xp : 32 * xp + 32, :].astype(BF)
            xsend[yp, xp, 32:64, :] = part[128 + 32 * xp : 160 + 32 * xp, :].astype(BF)
            xsend[yp, xp, 64:80, :] = (tail[yp * NX + xp] + sums).astype(BF)
        for dx in (2, 1, 3):
            xp = (x + dx) % NX
            pltpu.make_async_remote_copy(
                src_ref=xsend.at[yp, xp], dst_ref=xrecv.at[yp, x], send_sem=bx_s, recv_sem=bx_r.at[yp, x],
                device_id=(me_ep, y * NX + xp), device_id_type=MESH,
            ).start()

    total = None
    for dy in DYS:
        yp = (y + dy) % NY
        acc = xsend[yp, x].astype(F32)
        for dx in (1, 3, 2):
            xp = (x + dx) % NX
            pltpu.make_async_remote_copy(
                src_ref=xsend.at[yp, xp], dst_ref=xrecv.at[yp, xp], send_sem=bx_s, recv_sem=bx_r.at[yp, xp],
                device_id=(me_ep, y * NX + xp), device_id_type=MESH,
            ).wait_recv()
            acc = acc + xrecv[yp, xp].astype(F32)
        if dy == 0:
            total = acc
        else:
            end = acc[64:80, :]
            lost = end - end.astype(BF).astype(F32)
            lost = jnp.where((sub == 9) | (sub == 11), pltpu.roll(lost, 1, 0), 0.0)
            ysend[yp, 0:64, :] = acc[0:64, :].astype(BF)
            ysend[yp, 64:80, :] = (end + lost).astype(BF)
            pltpu.make_async_remote_copy(
                src_ref=ysend.at[yp], dst_ref=yrecv.at[y], send_sem=by_s, recv_sem=by_r.at[y],
                device_id=(me_ep, yp * NX + x), device_id_type=MESH,
            ).start()

    for dy in (1, 7, 2, 6, 3, 5, 4):
        yp = (y + dy) % NY
        pltpu.make_async_remote_copy(
            src_ref=ysend.at[yp], dst_ref=yrecv.at[yp], send_sem=by_s, recv_sem=by_r.at[yp],
            device_id=(me_ep, yp * NX + x), device_id_type=MESH,
        ).wait_recv()
        total = total + yrecv[yp].astype(F32)

    scale = lax.rsqrt((total[72:73, :] + total[73:74, :]) / D + EPS)
    own_scale = lax.rsqrt((total[74:75, :] + total[75:76, :]) / D + EPS)
    gate_v = total[0:32, :] * scale
    hid[me_tp] = (gate_v / (1.0 + jnp.exp(-gate_v)) * (total[32:64, :] * scale)).astype(BF)
    gate_s = total[64:68, :] * own_scale
    hsh[me_tp] = (gate_s / (1.0 + jnp.exp(-gate_s)) * (total[68:72, :] * own_scale)).astype(BF)

    def hidden_copies(p, to, sem_slot):
        return (
            pltpu.make_async_remote_copy(
                src_ref=hid.at[p], dst_ref=hid.at[p], send_sem=c_s, recv_sem=c_r.at[sem_slot],
                device_id=(me_ep, to), device_id_type=MESH,
            ),
            pltpu.make_async_remote_copy(
                src_ref=hsh.at[p], dst_ref=hsh.at[p], send_sem=cs_s, recv_sem=cs_r.at[sem_slot],
                device_id=(me_ep, to), device_id_type=MESH,
            ),
        )

    for dy in DYS[:-1]:
        for copy in hidden_copies(me_tp, ((y + dy) % NY) * NX + x, me_tp):
            copy.start()
    for dy in (0, 1, 7, 2, 6, 3, 5, 4):
        p = ((y + dy) % NY) * NX + x
        if dy != 0:
            for copy in hidden_copies(p, p, p):
                copy.wait_recv()
        for dx in (2, 1, 3):
            for copy in hidden_copies(p, y * NX + (x + dx) % NX, p):
                copy.start()
    for dy in (0, 1, 7, 2, 6, 3, 5, 4):
        for dx in (1, 3, 2):
            p = ((y + dy) % NY) * NX + (x + dx) % NX
            for copy in hidden_copies(p, y * NX + (x + dx) % NX, p):
                copy.wait_recv()

    both = dot(dt[...], hid[...].reshape(1024, 128))
    back = jnp.where((r1 // 2) % 2 == 0, both[0:128, :], both[128:256, :])
    rows[...] = back.T
    for b in range(NEP):
        dsend[b] = rows[4 * b : 4 * b + 4, :].astype(BF)

    def give_back(i, carry):
        to = ep_target(i, z, c)
        pltpu.make_async_remote_copy(
            src_ref=dsend.at[to], dst_ref=drecv.at[me_ep], send_sem=d_s, recv_sem=d_r,
            device_id=(to, me_tp), device_id_type=MESH,
        ).start()
        return carry

    lax.fori_loop(0, 31, give_back, 0)
    drecv[me_ep] = dsend[me_ep]

    for p in range(NTP):
        rows[4 * p : 4 * p + 4, :] = hsh[p].astype(F32)
    turned = rows[...].T
    shared_out = jnp.zeros((16, 128), F32)
    for g in range(8):
        shared_out = shared_out + dot(turned[16 * g : 16 * g + 16, :].astype(BF), sd[128 * g : 128 * g + 128, :])
    w_hi = weight.astype(BF)
    rest = weight - w_hi.astype(F32)
    w_mid = rest.astype(BF)
    w_lo = (rest - w_mid.astype(F32)).astype(BF)

    pltpu.make_async_copy(drecv.at[pl.ds(0, 31)], drecv.at[pl.ds(0, 31)], d_r).wait()
    for b in range(NEP):
        rows[4 * b : 4 * b + 4, :] = drecv[b].astype(F32)
    given = rows[...].astype(BF)
    combined = dot(w_hi, given) + dot(w_mid, given) + dot(w_lo, given) + shared_out

    out_squares = jnp.sum(combined * combined, axis=1, keepdims=True)
    out_line = jnp.sum(jnp.where(lane == sub, out_squares, 0.0), axis=0, keepdims=True)
    esend[...] = out_line

    def tell(i, carry):
        to = tp_target(i, y, x)
        pltpu.make_async_remote_copy(
            src_ref=esend, dst_ref=erecv.at[me_tp], send_sem=e_s, recv_sem=e_r,
            device_id=(me_ep, to), device_id_type=MESH,
        ).start()
        return carry

    lax.fori_loop(0, 31, tell, 0)
    erecv[me_tp] = out_line
    pltpu.make_async_copy(erecv.at[pl.ds(0, 31)], erecv.at[pl.ds(0, 31)], e_r).wait()
    all_squares = jnp.sum(erecv[...], axis=0)
    column = jnp.sum(jnp.where(lane == sub, all_squares, 0.0), axis=1, keepdims=True)
    out_scale = lax.rsqrt(column / D + EPS)
    out_ref[...] = (combined * out_scale * og[...].astype(F32)).astype(BF)

    for ref, sem in (
        (asend.at[pl.ds(0, 31)], a_s), (xsend.at[pl.ds(0, 6)], bx_s), (ysend.at[pl.ds(0, 7)], by_s),
        (hid.at[pl.ds(0, 31)], c_s), (hsh.at[pl.ds(0, 31)], cs_s), (dsend.at[pl.ds(0, 31)], d_s),
        (erecv.at[pl.ds(0, 31)], e_s),
    ):
        pltpu.make_async_copy(ref, ref, sem).wait()


def solution(mesh):
    def on_device(tokens, routes, gates, pre_gain, eg, eu, ed, sg, su, sd, out_gain):
        dma = pltpu.SemaphoreType.DMA
        return pl.pallas_call(
            kernel,
            name="experts",
            out_shape=jax.ShapeDtypeStruct((16, 128), BF),
            in_specs=[pl.BlockSpec(memory_space=pl.ANY)] * 11,
            out_specs=pl.BlockSpec(memory_space=pltpu.VMEM),
            scratch_shapes=[
                pltpu.VMEM((16, 128), BF), pltpu.VMEM((16, 4), jnp.int32), pltpu.VMEM((16, 4), F32),
                pltpu.VMEM((1, 128), BF), pltpu.VMEM((2, 128, 1024), BF), pltpu.VMEM((2, 128, 1024), BF),
                pltpu.VMEM((2, 1024, 128), BF), pltpu.VMEM((128, 1024), BF), pltpu.VMEM((128, 1024), BF),
                pltpu.VMEM((1024, 128), BF), pltpu.VMEM((1, 128), BF),
                pltpu.VMEM((8, 256, 256), BF), pltpu.VMEM((256, 1024), BF), pltpu.VMEM((256, 1024), BF),
                pltpu.VMEM((32, 4, 128), BF), pltpu.VMEM((32, 4, 128), BF), pltpu.VMEM((128, 128), F32),
                pltpu.VMEM((32, 16, 128), F32), pltpu.VMEM((128, 256), BF), pltpu.VMEM((128, 1024), BF),
                pltpu.VMEM((8, 4, 80, 128), BF), pltpu.VMEM((8, 4, 80, 128), BF),
                pltpu.VMEM((8, 80, 128), BF), pltpu.VMEM((8, 80, 128), BF),
                pltpu.VMEM((32, 32, 128), BF), pltpu.VMEM((32, 4, 128), BF),
                pltpu.VMEM((32, 4, 128), BF), pltpu.VMEM((32, 4, 128), BF),
                pltpu.VMEM((1, 128), F32), pltpu.VMEM((32, 1, 128), F32),
                dma((11,)), dma, dma, dma, dma((8, 4)), dma, dma((8,)), dma, dma((32,)), dma, dma((32,)),
                dma, dma, dma, dma,
            ],
            compiler_params=pltpu.CompilerParams(collective_id=0, has_side_effects=True),
        )(tokens, routes, gates, pre_gain.reshape(1, 128), eg, eu, ed, sg, su, sd, out_gain.reshape(1, 128))

    return jax.shard_map(
        on_device,
        mesh=mesh,
        in_specs=(
            P("ep", "tp"), P("ep", None), P("ep", None), P("tp"), P("ep", "tp", None), P("ep", "tp", None),
            P("ep", None, "tp"), P("tp", None), P("tp", None), P(None, "tp"), P("tp"),
        ),
        out_specs=P("ep", "tp"),
        check_vma=False,
    )
```

```python
import jax
import jax.numpy as jnp
from jax import lax
from jax.experimental import pallas as pl
from jax.experimental.pallas import tpu as pltpu
from jax.sharding import PartitionSpec as P

MESH = pl.DeviceIdType.MESH
BF = jnp.bfloat16
F32 = jnp.float32
D = 4096.0
EPS = 1e-06
NX, NY, NZ = 4, 8, 16
NEP, NTP = 32, 32
FAR_Z = (8, 7, 9, 6, 10, 5, 11, 4, 12, 3, 13, 2, 14, 1, 15, 0)
FAR_Y = (4, 3, 5, 2, 6, 1, 7, 0)
NEAR_Y = (0, 1, 7, 2, 6, 3, 5, 4)
FAR_X = (2, 1, 3, 0)
NT = (((1,), (1,)), ((), ()))
NN = (((1,), (0,)), ((), ()))


def dot(a, b, dims=NN):
    return lax.dot_general(a, b, dims, preferred_element_type=F32)


def silu(v):
    return v / (1.0 + jnp.exp(-v))


def kernel(
    tok_h, routes_h, gates_h, pg_h, eg_h, eu_h, ed_h, sg_h, su_h, sd_h, og_h,
    out_ref,
    tok, routes, gates, pg, eg, eu, ed, sg, su, sd, og,
    wt, swt, dt, asend, arecv, rows, xbd, sxbd,
    ssend, srecv, hsh, xsend, xrecv, ysend, yrecv, qsend, qrecv, hid, dsend, drecv, esend, erecv,
    in_sem, a_s, a_r, s_s, s_r, h_s, h_r, bx_s, bx_r, by_s, by_r, q_s, q_r, c_s, c_r, d_s, d_r, e_s, e_r,
):
    me_ep, me_tp = lax.axis_index("ep"), lax.axis_index("tp")
    z, c = me_ep // 2, me_ep % 2
    y, x = me_tp // NX, me_tp % NX
    zs = {d: (z + d) % NZ for d in FAR_Z}
    ys = {d: (y + d) % NY for d in FAR_Y}
    xs = {d: (x + d) % NX for d in FAR_X}
    far_ep = [2 * zs[d] + (c if same else 1 - c) for d in FAR_Z for same in (0, 1) if d or not same]
    far_tp = [NX * ys[dy] + xs[dx] for dy in FAR_Y for dx in FAR_X if dy or dx]

    def send(src, dst, send_sem, recv_sem, ep=None, tp=None):
        return pltpu.make_async_remote_copy(
            src_ref=src, dst_ref=dst, send_sem=send_sem, recv_sem=recv_sem,
            device_id=(me_ep if ep is None else ep, me_tp if tp is None else tp), device_id_type=MESH,
        )

    def wait_bytes(ref, sem):
        pltpu.make_async_copy(ref, ref, sem).wait()

    pairs = (
        (tok_h, tok), (routes_h, routes), (gates_h, gates), (pg_h, pg), (og_h, og),
        (eg_h, eg), (eu_h, eu), (sg_h, sg), (su_h, su), (ed_h, ed), (sd_h, sd),
    )
    loads = [pltpu.make_async_copy(a, b, in_sem.at[k]) for k, (a, b) in enumerate(pairs)]
    for load in loads[:3]:
        load.start()
    barrier = pltpu.get_barrier_semaphore()
    for to in far_ep:
        pl.semaphore_signal(barrier, inc=1, device_id=(to, me_tp), device_id_type=MESH)
    for to in far_tp:
        pl.semaphore_signal(barrier, inc=1, device_id=(me_ep, to), device_id_type=MESH)
    for load in loads[3:]:
        load.start()
    for load in loads[:5]:
        load.wait()

    lane = lax.broadcasted_iota(jnp.int32, (16, 128), 1)
    sub = lax.broadcasted_iota(jnp.int32, (16, 128), 0)
    row = lax.broadcasted_iota(jnp.int32, (128, 16), 0)
    named = jnp.zeros((128, 16), F32)
    weight = jnp.zeros((128, 16), F32)
    for k in range(4):
        hit = routes[k : k + 1, :] == row // 2
        named = named + jnp.where(hit, 1.0, 0.0)
        weight = weight + jnp.where(hit, gates[k : k + 1, :], 0.0)
    earlier = jnp.where(
        lax.broadcasted_iota(jnp.int32, (16, 16), 0) < lax.broadcasted_iota(jnp.int32, (16, 16), 1), 1.0, 0.0
    )
    slot = dot(named.astype(BF), earlier.astype(BF))
    chosen = (named > 0.5) & (jnp.abs(slot - (row % 2).astype(F32)) < 0.5)
    select = jnp.where(chosen, 1.0, 0.0)
    weight = jnp.where(chosen, weight, 0.0).T
    w_hi = weight.astype(BF)
    rest = weight - w_hi.astype(F32)
    w_mid = rest.astype(BF)
    w_lo = (rest - w_mid.astype(F32)).astype(BF)
    own = tok[...]
    rows[...] = dot(select.astype(BF), own)
    for b in range(NEP):
        asend[b] = rows[4 * b : 4 * b + 4, :].astype(BF)
    arecv[me_ep] = asend[me_ep]

    for load in loads[5:]:
        load.wait()
    for k in range(8):
        for s, source in enumerate((eg, eu)):
            for e in range(2):
                at = 128 * (2 * s + e)
                wt[k, :, at : at + 128] = source[e, :, 128 * k : 128 * k + 128].T
        for half, source in enumerate((sg, su)):
            swt[128 * half : 128 * half + 128, 128 * k : 128 * k + 128] = source[:, 128 * k : 128 * k + 128].T
    for e in range(2):
        for half in range(2):
            for k in range(4):
                units = [ed[e, 32 * p + 16 * half : 32 * p + 16 * half + 16, :] for p in range(8 * k, 8 * k + 8)]
                at = 128 * (2 * half + e)
                dt[at : at + 128, 128 * k : 128 * k + 128] = jnp.concatenate(units, axis=0).T
    gain = pg[...].astype(F32)
    own32 = own.astype(F32)
    sxbd[...] = jnp.zeros_like(sxbd)
    own_gained = (own32 * gain).astype(BF)
    for g in range(8):
        sxbd[16 * g : 16 * g + 16, 128 * g : 128 * g + 128] = own_gained
    shared_part = dot(swt[...], sxbd[...], NT)
    own_squares = jnp.sum(own32 * own32, axis=1, keepdims=True)
    own_line = jnp.sum(jnp.where(lane % 16 == sub, own_squares, 0.0), axis=0, keepdims=True)
    own_line_hi = own_line.astype(BF).astype(F32)
    own_sums = jnp.where(sub == 8, own_line_hi, 0.0) + jnp.where(sub == 9, own_line - own_line_hi, 0.0)
    for p in range(NTP):
        rows[0:4, :] = shared_part[4 * p : 4 * p + 4, :]
        rows[4:8, :] = shared_part[128 + 4 * p : 132 + 4 * p, :]
        rows[8:16, :] = own_sums[8:16, :]
        ssend[p] = rows[0:16, :].astype(BF)
    srecv[me_tp] = ssend[me_tp]

    pl.semaphore_wait(barrier, 62)
    for to in far_ep:
        send(asend.at[to], arecv.at[me_ep], a_s, a_r.at[z // 8], ep=to).start()
    for to in far_tp:
        send(ssend.at[to], srecv.at[me_tp], s_s, s_r, tp=to).start()

    r0 = lax.broadcasted_iota(jnp.int32, (64, 128), 0)
    r1 = lax.broadcasted_iota(jnp.int32, (64, 128), 1)
    first = (r0 // 2) % 2 == 0

    def rows_came(ch):
        @pl.when(z // 8 == ch)
        def _():
            wait_bytes(arecv.at[pl.ds(0, 15)], a_r.at[ch])

        @pl.when(z // 8 != ch)
        def _():
            wait_bytes(arecv.at[pl.ds(0, 16)], a_r.at[ch])

    def rows_multiplied(ch):
        for b in range(16):
            rows[4 * b : 4 * b + 4, :] = arecv[16 * ch + b].astype(F32)
        came = rows[0:64, :]
        squares = jnp.sum(came * came, axis=1, keepdims=True)
        line = jnp.sum(jnp.where(r1 % 64 == r0, squares, 0.0), axis=0, keepdims=True)
        gained = came * gain
        e0 = jnp.where(first, gained, 0.0).astype(BF)
        e1 = jnp.where(first, 0.0, gained).astype(BF)
        xbd[ch, 0:64, 0:128] = e0
        xbd[ch, 0:64, 128:256] = e1
        xbd[ch, 0:64, 256:512] = jnp.zeros((64, 256), BF)
        xbd[ch, 64:128, 0:256] = jnp.zeros((64, 256), BF)
        xbd[ch, 64:128, 256:384] = e0
        xbd[ch, 64:128, 384:512] = e1
        qsend[ch] = line
        qrecv[ch, me_tp] = line
        for some in (FAR_Y[:4], FAR_Y[4:]):
            for dy in some:
                part = dot(wt[ys[dy]], xbd[ch], NT)
                for xp in range(NX):
                    xsend[ch, ys[dy] * NX + xp] = part[32 * xp : 32 * xp + 32, :].astype(BF)
            for dy in some:
                yp = ys[dy]
                for dx in (2, 1, 3):
                    xp = xs[dx]
                    send(xsend.at[ch, yp * NX + xp], xrecv.at[ch, yp * NX + x], bx_s.at[ch], bx_r.at[ch, FAR_Y.index(dy) // 2], tp=y * NX + xp).start()
        for to in far_tp:
            send(qsend.at[ch], qrecv.at[ch, me_tp], q_s.at[ch], q_r.at[ch], tp=to).start()

    def summed_over_x(ch):
        total = None
        for at, dy in enumerate(FAR_Y):
            yp = ys[dy]
            if at % 2 == 0:
                wait_bytes(xrecv.at[ch, pl.ds(0, 6)], bx_r.at[ch, at // 2])
            acc = xsend[ch, yp * NX + x].astype(F32)
            for dx in (1, 3, 2):
                acc = acc + xrecv[ch, yp * NX + xs[dx]].astype(F32)
            if dy == 0:
                total = acc
            else:
                ysend[ch, yp] = acc.astype(BF)
                send(ysend.at[ch, yp], yrecv.at[ch, y], by_s.at[ch], by_r.at[ch], tp=yp * NX + x).start()
        return total

    def summed_over_y(ch, total):
        wait_bytes(yrecv.at[ch, pl.ds(0, 7)], by_r.at[ch])
        for dy in NEAR_Y[1:]:
            yp = ys[dy]
            total = total + yrecv[ch, yp].astype(F32)
        wait_bytes(qrecv.at[ch, pl.ds(0, 31)], q_r.at[ch])
        scale = lax.rsqrt(jnp.sum(qrecv[ch], axis=0) / D + EPS)
        v = total * scale
        h = silu(v) * pltpu.roll(v, 64, 1)
        hid[ch, me_tp] = jnp.where(lane < 64, h[0:16, :], pltpu.roll(h[16:32, :], 64, 1)).astype(BF)
        for to in far_tp:
            send(hid.at[ch, me_tp], hid.at[ch, me_tp], c_s.at[ch], c_r.at[ch], tp=to).start()

    def gathered(ch):
        wait_bytes(hid.at[ch, pl.ds(0, 31)], c_r.at[ch])

    def given_back(ch):
        both = dot(dt[...], hid[ch].reshape(512, 128))
        even = (lax.broadcasted_iota(jnp.int32, (128, 128), 1) // 2) % 2 == 0
        low = jnp.where(even, both[0:128, :], both[128:256, :])
        high = jnp.where(even, both[256:384, :], both[384:512, :])
        rows[...] = (low + pltpu.roll(high, 64, 1)).T
        for b in range(16):
            dsend[16 * ch + b] = rows[4 * b : 4 * b + 4, :].astype(BF)
        for b in range(16 * ch, 16 * ch + 16):
            @pl.when(me_ep != b)
            def _():
                send(dsend.at[b], drecv.at[me_ep], d_s, d_r, ep=b).start()

    rows_came(0)
    rows_multiplied(0)
    total0 = summed_over_x(0)
    rows_came(1)
    rows_multiplied(1)
    summed_over_y(0, total0)

    wait_bytes(srecv.at[pl.ds(0, 31)], s_r)
    shared_sum = jnp.sum(srecv[...].astype(F32), axis=0)
    own_scale = lax.rsqrt((shared_sum[8:9, :] + shared_sum[9:10, :]) / D + EPS)
    hsh[me_tp] = (silu(shared_sum[0:4, :] * own_scale) * (shared_sum[4:8, :] * own_scale)).astype(BF)
    for to in far_tp:
        send(hsh.at[me_tp], hsh.at[me_tp], h_s, h_r, tp=to).start()

    total1 = summed_over_x(1)
    summed_over_y(1, total1)
    gathered(0)
    given_back(0)
    gathered(1)
    given_back(1)
    drecv[me_ep] = dsend[me_ep]

    wait_bytes(hsh.at[pl.ds(0, 31)], h_r)
    for p in range(NTP):
        rows[4 * p : 4 * p + 4, :] = hsh[p].astype(F32)
    turned = rows[...].T.astype(BF)
    shared_out = jnp.zeros((16, 128), F32)
    for g in range(8):
        shared_out = shared_out + dot(turned[16 * g : 16 * g + 16, :], sd[128 * g : 128 * g + 128, :])

    wait_bytes(drecv.at[pl.ds(0, 31)], d_r)
    for b in range(NEP):
        rows[4 * b : 4 * b + 4, :] = drecv[b].astype(F32)
    given = rows[...].astype(BF)
    combined = dot(w_hi, given) + dot(w_mid, given) + dot(w_lo, given) + shared_out
    out_squares = jnp.sum(combined * combined, axis=1, keepdims=True)
    out_line = jnp.sum(jnp.where(lane == sub, out_squares, 0.0), axis=0, keepdims=True)
    esend[...] = out_line
    for to in far_tp:
        send(esend, erecv.at[me_tp], e_s, e_r, tp=to).start()
    erecv[me_tp] = out_line
    wait_bytes(erecv.at[pl.ds(0, 31)], e_r)
    all_squares = jnp.sum(erecv[...], axis=0)
    column = jnp.sum(jnp.where(lane == sub, all_squares, 0.0), axis=1, keepdims=True)
    out_scale = lax.rsqrt(column / D + EPS)
    out_ref[...] = (combined * out_scale * og[...].astype(F32)).astype(BF)

    for ref, sem in (
        (asend.at[pl.ds(0, 31)], a_s), (ssend.at[pl.ds(0, 31)], s_s), (hsh.at[pl.ds(0, 31)], h_s),
        (dsend.at[pl.ds(0, 31)], d_s), (erecv.at[pl.ds(0, 31)], e_s),
    ):
        wait_bytes(ref, sem)
    for ch in range(2):
        wait_bytes(xsend.at[ch, pl.ds(0, 24)], bx_s.at[ch])
        wait_bytes(ysend.at[ch, pl.ds(0, 7)], by_s.at[ch])
        wait_bytes(hid.at[ch, pl.ds(0, 31)], c_s.at[ch])
        wait_bytes(qrecv.at[ch, pl.ds(0, 31)], q_s.at[ch])


def solution(mesh):
    def on_device(tokens, routes, gates, pre_gain, eg, eu, ed, sg, su, sd, out_gain):
        dma = pltpu.SemaphoreType.DMA
        return pl.pallas_call(
            kernel,
            name="experts",
            out_shape=jax.ShapeDtypeStruct((16, 128), BF),
            in_specs=[pl.BlockSpec(memory_space=pl.ANY)] * 11,
            out_specs=pl.BlockSpec(memory_space=pltpu.VMEM),
            scratch_shapes=[
                pltpu.VMEM((16, 128), BF), pltpu.VMEM((4, 16), jnp.int32), pltpu.VMEM((4, 16), F32),
                pltpu.VMEM((1, 128), BF), pltpu.VMEM((2, 128, 1024), BF), pltpu.VMEM((2, 128, 1024), BF),
                pltpu.VMEM((2, 1024, 128), BF), pltpu.VMEM((128, 1024), BF), pltpu.VMEM((128, 1024), BF),
                pltpu.VMEM((1024, 128), BF), pltpu.VMEM((1, 128), BF),
                pltpu.VMEM((8, 128, 512), BF), pltpu.VMEM((256, 1024), BF), pltpu.VMEM((512, 512), BF),
                pltpu.VMEM((32, 4, 128), BF), pltpu.VMEM((32, 4, 128), BF), pltpu.VMEM((128, 128), F32),
                pltpu.VMEM((2, 128, 512), BF), pltpu.VMEM((128, 1024), BF),
                pltpu.VMEM((32, 16, 128), BF), pltpu.VMEM((32, 16, 128), BF), pltpu.VMEM((32, 4, 128), BF),
                pltpu.VMEM((2, 32, 32, 128), BF), pltpu.VMEM((2, 32, 32, 128), BF),
                pltpu.VMEM((2, 8, 32, 128), BF), pltpu.VMEM((2, 8, 32, 128), BF),
                pltpu.VMEM((2, 1, 128), F32), pltpu.VMEM((2, 32, 1, 128), F32),
                pltpu.VMEM((2, 32, 16, 128), BF),
                pltpu.VMEM((32, 4, 128), BF), pltpu.VMEM((32, 4, 128), BF),
                pltpu.VMEM((1, 128), F32), pltpu.VMEM((32, 1, 128), F32),
                dma((11,)), dma, dma((2,)), dma, dma, dma, dma, dma((2,)), dma((2, 4)), dma((2,)), dma((2,)),
                dma((2,)), dma((2,)), dma((2,)), dma((2,)), dma, dma, dma, dma,
            ],
            compiler_params=pltpu.CompilerParams(collective_id=0, has_side_effects=True),
        )(tokens, routes.T, gates.T, pre_gain.reshape(1, 128), eg, eu, ed, sg, su, sd, out_gain.reshape(1, 128))

    return jax.shard_map(
        on_device,
        mesh=mesh,
        in_specs=(
            P("ep", "tp"), P("ep", None), P("ep", None), P("tp"), P("ep", "tp", None), P("ep", "tp", None),
            P("ep", None, "tp"), P("tp", None), P("tp", None), P(None, "tp"), P("tp"),
        ),
        out_specs=P("ep", "tp"),
        check_vma=False,
    )
```

```python
import jax
import jax.numpy as jnp
from jax import lax
from jax.experimental import pallas as pl
from jax.experimental.pallas import tpu as pltpu
from jax.sharding import PartitionSpec as P

MESH = pl.DeviceIdType.MESH
BF = jnp.bfloat16
F32 = jnp.float32
D = 4096.0
EPS = 1e-06
NX, NY, NZ = 4, 8, 16
NEP, NTP = 32, 32
FAR_Z = (8, 7, 9, 6, 10, 5, 11, 4, 12, 3, 13, 2, 14, 1, 15, 0)
FAR_Y = (4, 3, 5, 2, 6, 1, 7, 0)
NEAR_Y = (0, 1, 7, 2, 6, 3, 5, 4)
FAR_X = (2, 1, 3, 0)
STAGES = ((4, 3, 5), (2, 6, 1, 7, 0))
NT = (((1,), (1,)), ((), ()))
NN = (((1,), (0,)), ((), ()))


def dot(a, b, dims=NN):
    return lax.dot_general(a, b, dims, preferred_element_type=F32)


def silu(v):
    return v / (1.0 + jnp.exp(-v))


def kernel(
    tok_h, routes, gates, pg, eg_h, eu_h, ed_h, sg_h, su_h, sd_h, og,
    out_ref,
    tok, eg, eu, ed, sg, su, sd,
    wt, swt, dt, asend, arecv, rows, xsm, xbd, sxbd,
    ssend, srecv, hsh, bsend, brecv, xsend, xrecv, ysend, yrecv, qsend, qrecv, hid, dsend, drecv, esend, erecv,
    in_sem, a_s, a_r, s_s, s_r, h_s, h_r, b_s, b_r, bx_s, bx_r, by_s, by_r, q_s, q_r, c_s, c_r, d_s, d_r, e_s, e_r,
):
    me_ep, me_tp = lax.axis_index("ep"), lax.axis_index("tp")
    z, c = me_ep // 2, me_ep % 2
    y, x = me_tp // NX, me_tp % NX
    zs = {d: (z + d) % NZ for d in FAR_Z}
    ys = {d: (y + d) % NY for d in FAR_Y}
    xs = {d: (x + d) % NX for d in FAR_X}
    far_ep = [2 * zs[d] + (c if same else 1 - c) for d in FAR_Z for same in (0, 1) if d or not same]
    far_tp = [NX * ys[dy] + xs[dx] for dy in FAR_Y for dx in FAR_X if dy or dx]

    def send(src, dst, send_sem, recv_sem, ep=None, tp=None):
        return pltpu.make_async_remote_copy(
            src_ref=src, dst_ref=dst, send_sem=send_sem, recv_sem=recv_sem,
            device_id=(me_ep if ep is None else ep, me_tp if tp is None else tp), device_id_type=MESH,
        )

    def wait_bytes(ref, sem):
        pltpu.make_async_copy(ref, ref, sem).wait()

    pairs = (
        (tok_h, tok), (eg_h, eg), (eu_h, eu), (sg_h, sg), (su_h, su), (ed_h, ed), (sd_h, sd),
    )
    loads = [pltpu.make_async_copy(a, b, in_sem.at[k]) for k, (a, b) in enumerate(pairs)]
    loads[0].start()
    barrier = pltpu.get_barrier_semaphore()
    for to in far_ep:
        pl.semaphore_signal(barrier, inc=1, device_id=(to, me_tp), device_id_type=MESH)
    for to in far_tp:
        pl.semaphore_signal(barrier, inc=1, device_id=(me_ep, to), device_id_type=MESH)
    for load in loads[1:]:
        load.start()
    loads[0].wait()

    lane = lax.broadcasted_iota(jnp.int32, (16, 128), 1)
    sub = lax.broadcasted_iota(jnp.int32, (16, 128), 0)
    row = lax.broadcasted_iota(jnp.int32, (128, 16), 0)
    named = jnp.zeros((128, 16), F32)
    weight = jnp.zeros((128, 16), F32)
    for k in range(4):
        hit = routes[k : k + 1, :] == row // 2
        named = named + jnp.where(hit, 1.0, 0.0)
        weight = weight + jnp.where(hit, gates[k : k + 1, :], 0.0)
    earlier = jnp.where(
        lax.broadcasted_iota(jnp.int32, (16, 16), 0) < lax.broadcasted_iota(jnp.int32, (16, 16), 1), 1.0, 0.0
    )
    slot = dot(named.astype(BF), earlier.astype(BF))
    chosen = (named > 0.5) & (jnp.abs(slot - (row % 2).astype(F32)) < 0.5)
    select = jnp.where(chosen, 1.0, 0.0)
    weight = jnp.where(chosen, weight, 0.0).T
    w_hi = weight.astype(BF)
    rest = weight - w_hi.astype(F32)
    w_mid = rest.astype(BF)
    w_lo = (rest - w_mid.astype(F32)).astype(BF)
    own = tok[...]
    rows[...] = dot(select.astype(BF), own)
    for b in range(NEP):
        asend[b] = rows[4 * b : 4 * b + 4, :].astype(BF)
    arecv[me_ep] = asend[me_ep]

    for load in loads[1:]:
        load.wait()
    for k in range(8):
        for s, source in enumerate((eg, eu)):
            for e in range(2):
                at = 128 * (2 * s + e)
                turned = source[e, :, 128 * k : 128 * k + 128].T
                for part in range(8):
                    to = 64 * (part % 2) + 16 * (part // 2)
                    wt[k, to : to + 16, at : at + 128] = turned[16 * part : 16 * part + 16, :]
        for half, source in enumerate((sg, su)):
            swt[128 * half : 128 * half + 128, 128 * k : 128 * k + 128] = source[:, 128 * k : 128 * k + 128].T
    for e in range(2):
        for half in range(2):
            for k in range(4):
                units = [ed[e, 32 * p + 16 * half : 32 * p + 16 * half + 16, :] for p in range(8 * k, 8 * k + 8)]
                at = 128 * (2 * half + e)
                dt[at : at + 128, 128 * k : 128 * k + 128] = jnp.concatenate(units, axis=0).T
    gain = pg[...].astype(F32)
    own32 = own.astype(F32)
    sxbd[...] = jnp.zeros_like(sxbd)
    xsm[...] = jnp.zeros_like(xsm)
    xbd[...] = jnp.zeros_like(xbd)
    own_gained = (own32 * gain).astype(BF)
    for g in range(8):
        sxbd[16 * g : 16 * g + 16, 128 * g : 128 * g + 128] = own_gained
    shared_part = dot(swt[...], sxbd[...], NT)
    own_squares = jnp.sum(own32 * own32, axis=1, keepdims=True)
    own_line = jnp.sum(jnp.where(lane % 16 == sub, own_squares, 0.0), axis=0, keepdims=True)
    own_line_hi = own_line.astype(BF).astype(F32)
    own_sums = jnp.where(sub == 8, own_line_hi, 0.0) + jnp.where(sub == 9, own_line - own_line_hi, 0.0)
    for p in range(NTP):
        rows[0:4, :] = shared_part[4 * p : 4 * p + 4, :]
        rows[4:8, :] = shared_part[128 + 4 * p : 132 + 4 * p, :]
        rows[8:16, :] = own_sums[8:16, :]
        ssend[p] = rows[0:16, :].astype(BF)
    srecv[me_tp] = ssend[me_tp]

    pl.semaphore_wait(barrier, 62)
    for to in far_ep:
        send(asend.at[to], arecv.at[me_ep], a_s, a_r.at[z // 4], ep=to).start()
    for to in far_tp:
        send(ssend.at[to], srecv.at[me_tp], s_s, s_r, tp=to).start()

    def rows_came(quarter):
        @pl.when(z // 4 == quarter)
        def _():
            wait_bytes(arecv.at[pl.ds(0, 7)], a_r.at[quarter])

        @pl.when(z // 4 != quarter)
        def _():
            wait_bytes(arecv.at[pl.ds(0, 8)], a_r.at[quarter])

    def rows_split(ch, start, blocks):
        count = 4 * blocks
        for b in range(blocks):
            rows[4 * b : 4 * b + 4, :] = arecv[start + b].astype(F32)
        came = rows[0:count, :]
        r0 = lax.broadcasted_iota(jnp.int32, (count, 128), 0)
        r1 = lax.broadcasted_iota(jnp.int32, (count, 128), 1)
        squares = jnp.sum(came * came, axis=1, keepdims=True)
        line = jnp.sum(jnp.where(r1 % count == r0, squares, 0.0), axis=0, keepdims=True)
        qsend[ch] = line
        qrecv[32 * ch + me_tp] = line
        gained = came * gain
        first = (r0 // 2) % 2 == 0
        return jnp.where(first, gained, 0.0).astype(BF), jnp.where(first, 0.0, gained).astype(BF)

    def squares_told(ch):
        for to in far_tp:
            send(qsend.at[ch], qrecv.at[32 * ch + me_tp], q_s, q_r.at[ch], tp=to).start()

    def small_multiplied(ch):
        e0, e1 = rows_split(ch, 8 * ch, 8)
        for half in range(2):
            for s in range(2):
                at = 64 * half + 32 * s
                xsm[ch, half, at : at + 32, 256 * s : 256 * s + 128] = e0
                xsm[ch, half, at : at + 32, 256 * s + 128 : 256 * s + 256] = e1
        for some in STAGES:
            low = jnp.concatenate([wt[ys[dy], 0:64, :] for dy in some], axis=0)
            high = jnp.concatenate([wt[ys[dy], 64:128, :] for dy in some], axis=0)
            part = dot(low, xsm[ch, 0], NT) + dot(high, xsm[ch, 1], NT)
            for k, dy in enumerate(some):
                for xp in range(NX):
                    at = 64 * k + 16 * xp
                    bsend[32 * ch + ys[dy] * NX + xp] = part[at : at + 16, :].astype(BF)
            for dy in some:
                for dx in FAR_X:
                    if dy or dx:
                        to = ys[dy] * NX + xs[dx]
                        send(bsend.at[32 * ch + to], brecv.at[32 * ch + me_tp], b_s, b_r.at[ch], tp=to).start()
        brecv[32 * ch + me_tp] = bsend[32 * ch + me_tp]
        squares_told(ch)

    def scale_of(ch):
        wait_bytes(qrecv.at[pl.ds(0, 31)], q_r.at[ch])
        return lax.rsqrt(jnp.sum(qrecv[32 * ch : 32 * ch + 32], axis=0) / D + EPS)

    def units_told(ch, units):
        hid[32 * ch + me_tp] = units.astype(BF)
        for to in far_tp:
            send(hid.at[32 * ch + me_tp], hid.at[32 * ch + me_tp], c_s, c_r.at[ch], tp=to).start()

    def small_summed(ch):
        wait_bytes(brecv.at[pl.ds(0, 31)], b_r.at[ch])
        total = jnp.sum(brecv[32 * ch : 32 * ch + 32].astype(F32), axis=0)
        v = total * scale_of(ch)
        units_told(ch, silu(v) * pltpu.roll(v, 96, 1))

    def large_multiplied():
        e0, e1 = rows_split(2, 16, 16)
        for s in range(2):
            xbd[64 * s : 64 * s + 64, 256 * s : 256 * s + 128] = e0
            xbd[64 * s : 64 * s + 64, 256 * s + 128 : 256 * s + 256] = e1
        for some in (FAR_Y[:4], FAR_Y[4:]):
            part = dot(jnp.concatenate([wt[ys[dy]] for dy in some], axis=0), xbd[...], NT)
            for k, dy in enumerate(some):
                for xp in range(NX):
                    at = 128 * k + 16 * xp
                    xsend[ys[dy] * NX + xp, 0:16, :] = part[at : at + 16, :].astype(BF)
                    xsend[ys[dy] * NX + xp, 16:32, :] = part[at + 64 : at + 80, :].astype(BF)
            for dy in some:
                yp = ys[dy]
                for dx in (2, 1, 3):
                    xp = xs[dx]
                    send(
                        xsend.at[yp * NX + xp], xrecv.at[yp * NX + x], bx_s, bx_r.at[FAR_Y.index(dy) // 4], tp=y * NX + xp
                    ).start()
        squares_told(2)

    def large_summed_over_x():
        total = None
        for at, dy in enumerate(FAR_Y):
            yp = ys[dy]
            if at % 4 == 0:
                wait_bytes(xrecv.at[pl.ds(0, 12)], bx_r.at[at // 4])
            acc = xsend[yp * NX + x].astype(F32)
            for dx in (1, 3, 2):
                acc = acc + xrecv[yp * NX + xs[dx]].astype(F32)
            if dy == 0:
                total = acc
            else:
                ysend[yp] = acc.astype(BF)
                send(ysend.at[yp], yrecv.at[y], by_s, by_r, tp=yp * NX + x).start()
        return total

    def large_summed_over_y(total):
        wait_bytes(yrecv.at[pl.ds(0, 7)], by_r)
        for dy in NEAR_Y[1:]:
            total = total + yrecv[ys[dy]].astype(F32)
        v = total * scale_of(2)
        h = silu(v) * pltpu.roll(v, 64, 1)
        units_told(2, jnp.where(lane < 64, h[0:16, :], pltpu.roll(h[16:32, :], 64, 1)))

    def given_back(ch, start, blocks):
        wait_bytes(hid.at[pl.ds(0, 31)], c_r.at[ch])
        both = dot(dt[...], hid[32 * ch : 32 * ch + 32].reshape(512, 128))
        even = (lax.broadcasted_iota(jnp.int32, (128, 128), 1) // 2) % 2 == 0
        low = jnp.where(even, both[0:128, :], both[128:256, :])
        high = jnp.where(even, both[256:384, :], both[384:512, :])
        rows[...] = (low + pltpu.roll(high, 64, 1)).T
        for b in range(blocks):
            dsend[start + b] = rows[4 * b : 4 * b + 4, :].astype(BF)
        for b in range(start, start + blocks):
            @pl.when(me_ep != b)
            def _():
                send(dsend.at[b], drecv.at[me_ep], d_s, d_r, ep=b).start()

    rows_came(0)
    small_multiplied(0)
    rows_came(2)
    rows_came(3)
    large_multiplied()
    rows_came(1)
    small_multiplied(1)
    small_summed(0)

    wait_bytes(srecv.at[pl.ds(0, 31)], s_r)
    shared_sum = jnp.sum(srecv[...].astype(F32), axis=0)
    own_scale = lax.rsqrt((shared_sum[8:9, :] + shared_sum[9:10, :]) / D + EPS)
    hsh[me_tp] = (silu(shared_sum[0:4, :] * own_scale) * (shared_sum[4:8, :] * own_scale)).astype(BF)
    for to in far_tp:
        send(hsh.at[me_tp], hsh.at[me_tp], h_s, h_r, tp=to).start()

    total2 = large_summed_over_x()
    small_summed(1)
    given_back(0, 0, 8)
    large_summed_over_y(total2)
    given_back(1, 8, 8)

    @pl.when(z // 8 == 0)
    def _():
        drecv[me_ep] = dsend[me_ep]

    @pl.when(z // 8 == 1)
    def _():
        given_back(2, 16, 16)
        drecv[me_ep] = dsend[me_ep]

    wait_bytes(hsh.at[pl.ds(0, 31)], h_r)
    for p in range(NTP):
        rows[4 * p : 4 * p + 4, :] = hsh[p].astype(F32)
    turned = rows[...].T.astype(BF)
    shared_out = jnp.zeros((16, 128), F32)
    for g in range(8):
        shared_out = shared_out + dot(turned[16 * g : 16 * g + 16, :], sd[128 * g : 128 * g + 128, :])

    wait_bytes(drecv.at[pl.ds(0, 31)], d_r)
    for b in range(NEP):
        rows[4 * b : 4 * b + 4, :] = drecv[b].astype(F32)
    given = rows[...].astype(BF)
    combined = dot(w_hi, given) + dot(w_mid, given) + dot(w_lo, given) + shared_out
    out_squares = jnp.sum(combined * combined, axis=1, keepdims=True)
    out_line = jnp.sum(jnp.where(lane == sub, out_squares, 0.0), axis=0, keepdims=True)
    esend[...] = out_line
    for to in far_tp:
        send(esend, erecv.at[me_tp], e_s, e_r, tp=to).start()
    erecv[me_tp] = out_line

    @pl.when(z // 8 == 0)
    def _():
        given_back(2, 16, 16)

    wait_bytes(erecv.at[pl.ds(0, 31)], e_r)
    all_squares = jnp.sum(erecv[...], axis=0)
    column = jnp.sum(jnp.where(lane == sub, all_squares, 0.0), axis=1, keepdims=True)
    out_scale = lax.rsqrt(column / D + EPS)
    out_ref[...] = (combined * out_scale * og[...].astype(F32)).astype(BF)

    for ref, sem in (
        (asend.at[pl.ds(0, 31)], a_s), (ssend.at[pl.ds(0, 31)], s_s), (hsh.at[pl.ds(0, 31)], h_s),
        (dsend.at[pl.ds(0, 31)], d_s), (erecv.at[pl.ds(0, 31)], e_s), (bsend.at[pl.ds(0, 62)], b_s),
        (xsend.at[pl.ds(0, 24)], bx_s), (ysend.at[pl.ds(0, 7)], by_s), (hid.at[pl.ds(0, 93)], c_s),
        (qrecv.at[pl.ds(0, 93)], q_s),
    ):
        wait_bytes(ref, sem)


def solution(mesh):
    def on_device(tokens, routes, gates, pre_gain, eg, eu, ed, sg, su, sd, out_gain):
        dma = pltpu.SemaphoreType.DMA
        hbm = pl.BlockSpec(memory_space=pl.ANY)
        vmem = pl.BlockSpec(memory_space=pltpu.VMEM)
        return pl.pallas_call(
            kernel,
            name="experts",
            out_shape=jax.ShapeDtypeStruct((16, 128), BF),
            in_specs=[hbm] + [vmem] * 3 + [hbm] * 6 + [vmem],
            out_specs=pl.BlockSpec(memory_space=pltpu.VMEM),
            scratch_shapes=[
                pltpu.VMEM((16, 128), BF), pltpu.VMEM((2, 128, 1024), BF), pltpu.VMEM((2, 128, 1024), BF),
                pltpu.VMEM((2, 1024, 128), BF), pltpu.VMEM((128, 1024), BF), pltpu.VMEM((128, 1024), BF),
                pltpu.VMEM((1024, 128), BF),
                pltpu.VMEM((8, 128, 512), BF), pltpu.VMEM((256, 1024), BF), pltpu.VMEM((512, 512), BF),
                pltpu.VMEM((32, 4, 128), BF), pltpu.VMEM((32, 4, 128), BF), pltpu.VMEM((128, 128), F32),
                pltpu.VMEM((2, 2, 128, 512), BF), pltpu.VMEM((128, 512), BF), pltpu.VMEM((128, 1024), BF),
                pltpu.VMEM((32, 16, 128), BF), pltpu.VMEM((32, 16, 128), BF), pltpu.VMEM((32, 4, 128), BF),
                pltpu.VMEM((64, 16, 128), BF), pltpu.VMEM((64, 16, 128), BF),
                pltpu.VMEM((32, 32, 128), BF), pltpu.VMEM((32, 32, 128), BF),
                pltpu.VMEM((8, 32, 128), BF), pltpu.VMEM((8, 32, 128), BF),
                pltpu.VMEM((3, 1, 128), F32), pltpu.VMEM((96, 1, 128), F32),
                pltpu.VMEM((96, 16, 128), BF),
                pltpu.VMEM((32, 4, 128), BF), pltpu.VMEM((32, 4, 128), BF),
                pltpu.VMEM((1, 128), F32), pltpu.VMEM((32, 1, 128), F32),
                dma((7,)), dma, dma((4,)), dma, dma, dma, dma, dma, dma((2,)), dma, dma((2,)), dma, dma,
                dma, dma((3,)), dma, dma((3,)), dma, dma, dma, dma,
            ],
            compiler_params=pltpu.CompilerParams(collective_id=0, has_side_effects=True, vmem_limit_bytes=55212 * 1024),
        )(tokens, routes.T, gates.T, pre_gain.reshape(1, 128), eg, eu, ed, sg, su, sd, out_gain.reshape(1, 128))

    return jax.shard_map(
        on_device,
        mesh=mesh,
        in_specs=(
            P("ep", "tp"), P("ep", None), P("ep", None), P("tp"), P("ep", "tp", None), P("ep", "tp", None),
            P("ep", None, "tp"), P("tp", None), P("tp", None), P(None, "tp"), P("tp"),
        ),
        out_specs=P("ep", "tp"),
        check_vma=False,
    )
```

```python
import jax
import jax.numpy as jnp
from jax import lax
from jax.experimental import pallas as pl
from jax.experimental.pallas import tpu as pltpu
from jax.sharding import PartitionSpec as P

MESH = pl.DeviceIdType.MESH
BF = jnp.bfloat16
F32 = jnp.float32
D = 4096.0
EPS = 1e-06
NX, NY, NZ = 4, 8, 16
NEP, NTP = 32, 32
FAR_Z = (8, 7, 9, 6, 10, 5, 11, 4, 12, 3, 13, 2, 14, 1, 15, 0)
FAR_Y = (4, 3, 5, 2, 6, 1, 7, 0)
NEAR_Y = (0, 1, 7, 2, 6, 3, 5, 4)
FAR_X = (2, 1, 3, 0)
STAGES = ((4,), (3, 5), (2, 6, 1, 7, 0))
NT = (((1,), (1,)), ((), ()))
NN = (((1,), (0,)), ((), ()))


def dot(a, b, dims=NN):
    return lax.dot_general(a, b, dims, preferred_element_type=F32)


def silu(v):
    return v / (1.0 + jnp.exp(-v))


def kernel(
    tok_h, routes, gates, pg, eg_h, eu_h, ed_h, sg_h, su_h, sd_h, og,
    out_ref,
    tok, eg, eu, ed, sg, su, sd,
    wt, swt, dt, asend, arecv, rows, xsm, xbd, sxbd,
    ssend, srecv, hsh, bsend, brecv, xsend, xrecv, ysend, yrecv, qsend, qrecv, hid, dsend, drecv, esend, erecv,
    in_sem, a_s, a_r, s_s, s_r, h_s, h_r, b_s, b_r, bx_s, bx_r, by_s, by_r, q_s, q_r, c_s, c_r, d_s, d_r, e_s, e_r,
):
    me_ep, me_tp = lax.axis_index("ep"), lax.axis_index("tp")
    z, c = me_ep // 2, me_ep % 2
    y, x = me_tp // NX, me_tp % NX
    zs = {d: (z + d) % NZ for d in FAR_Z}
    ys = {d: (y + d) % NY for d in FAR_Y}
    xs = {d: (x + d) % NX for d in FAR_X}
    far_ep = [2 * zs[d] + (c if same else 1 - c) for d in FAR_Z for same in (0, 1) if d or not same]
    far_tp = [NX * ys[dy] + xs[dx] for dy in FAR_Y for dx in FAR_X if dy or dx]

    def send(src, dst, send_sem, recv_sem, ep=None, tp=None):
        return pltpu.make_async_remote_copy(
            src_ref=src, dst_ref=dst, send_sem=send_sem, recv_sem=recv_sem,
            device_id=(me_ep if ep is None else ep, me_tp if tp is None else tp), device_id_type=MESH,
        )

    def wait_bytes(ref, sem):
        pltpu.make_async_copy(ref, ref, sem).wait()

    pairs = (
        (tok_h, tok), (eg_h, eg), (eu_h, eu), (sg_h, sg), (su_h, su), (ed_h, ed), (sd_h, sd),
    )
    loads = [pltpu.make_async_copy(a, b, in_sem.at[k]) for k, (a, b) in enumerate(pairs)]
    loads[0].start()
    barrier = pltpu.get_barrier_semaphore()
    for to in far_ep:
        pl.semaphore_signal(barrier, inc=1, device_id=(to, me_tp), device_id_type=MESH)
    for to in far_tp:
        pl.semaphore_signal(barrier, inc=1, device_id=(me_ep, to), device_id_type=MESH)
    for load in loads[1:]:
        load.start()
    loads[0].wait()

    lane = lax.broadcasted_iota(jnp.int32, (16, 128), 1)
    sub = lax.broadcasted_iota(jnp.int32, (16, 128), 0)
    row = lax.broadcasted_iota(jnp.int32, (128, 16), 0)
    named = jnp.zeros((128, 16), F32)
    weight = jnp.zeros((128, 16), F32)
    for k in range(4):
        hit = routes[k : k + 1, :] == row // 2
        named = named + jnp.where(hit, 1.0, 0.0)
        weight = weight + jnp.where(hit, gates[k : k + 1, :], 0.0)
    earlier = jnp.where(
        lax.broadcasted_iota(jnp.int32, (16, 16), 0) < lax.broadcasted_iota(jnp.int32, (16, 16), 1), 1.0, 0.0
    )
    slot = dot(named.astype(BF), earlier.astype(BF))
    chosen = (named > 0.5) & (jnp.abs(slot - (row % 2).astype(F32)) < 0.5)
    select = jnp.where(chosen, 1.0, 0.0)
    weight = jnp.where(chosen, weight, 0.0).T
    w_hi = weight.astype(BF)
    rest = weight - w_hi.astype(F32)
    w_mid = rest.astype(BF)
    w_lo = (rest - w_mid.astype(F32)).astype(BF)
    own = tok[...]
    rows[...] = dot(select.astype(BF), own)
    for b in range(NEP):
        asend[b] = rows[4 * b : 4 * b + 4, :].astype(BF)
    arecv[me_ep] = asend[me_ep]

    for load in loads[1:]:
        load.wait()
    for k in range(8):
        for s, source in enumerate((eg, eu)):
            for e in range(2):
                at = 128 * (2 * s + e)
                turned = source[e, :, 128 * k : 128 * k + 128].T
                for part in range(8):
                    to = 64 * (part % 2) + 16 * (part // 2)
                    wt[k, to : to + 16, at : at + 128] = turned[16 * part : 16 * part + 16, :]
        for half, source in enumerate((sg, su)):
            swt[128 * half : 128 * half + 128, 128 * k : 128 * k + 128] = source[:, 128 * k : 128 * k + 128].T
    for e in range(2):
        for half in range(2):
            for k in range(4):
                units = [ed[e, 32 * p + 16 * half : 32 * p + 16 * half + 16, :] for p in range(8 * k, 8 * k + 8)]
                at = 128 * (2 * half + e)
                dt[at : at + 128, 128 * k : 128 * k + 128] = jnp.concatenate(units, axis=0).T
    gain = pg[...].astype(F32)
    own32 = own.astype(F32)
    sxbd[...] = jnp.zeros_like(sxbd)
    xsm[...] = jnp.zeros_like(xsm)
    xbd[...] = jnp.zeros_like(xbd)
    own_gained = (own32 * gain).astype(BF)
    for g in range(8):
        sxbd[16 * g : 16 * g + 16, 128 * g : 128 * g + 128] = own_gained
    shared_part = dot(swt[...], sxbd[...], NT)
    own_squares = jnp.sum(own32 * own32, axis=1, keepdims=True)
    own_line = jnp.sum(jnp.where(lane % 16 == sub, own_squares, 0.0), axis=0, keepdims=True)
    own_line_hi = own_line.astype(BF).astype(F32)
    own_sums = jnp.where(sub == 8, own_line_hi, 0.0) + jnp.where(sub == 9, own_line - own_line_hi, 0.0)
    for p in range(NTP):
        rows[0:4, :] = shared_part[4 * p : 4 * p + 4, :]
        rows[4:8, :] = shared_part[128 + 4 * p : 132 + 4 * p, :]
        rows[8:16, :] = own_sums[8:16, :]
        ssend[p] = rows[0:16, :].astype(BF)
    srecv[me_tp] = ssend[me_tp]

    pl.semaphore_wait(barrier, 62)
    for to in far_ep:
        send(asend.at[to], arecv.at[me_ep], a_s, a_r.at[z // 4], ep=to).start()
    for to in far_tp:
        send(ssend.at[to], srecv.at[me_tp], s_s, s_r, tp=to).start()

    def rows_came(quarter):
        @pl.when(z // 4 == quarter)
        def _():
            wait_bytes(arecv.at[pl.ds(0, 7)], a_r.at[quarter])

        @pl.when(z // 4 != quarter)
        def _():
            wait_bytes(arecv.at[pl.ds(0, 8)], a_r.at[quarter])

    def rows_split(ch, start, blocks):
        count = 4 * blocks
        for b in range(blocks):
            rows[4 * b : 4 * b + 4, :] = arecv[start + b].astype(F32)
        came = rows[0:count, :]
        r0 = lax.broadcasted_iota(jnp.int32, (count, 128), 0)
        r1 = lax.broadcasted_iota(jnp.int32, (count, 128), 1)
        squares = jnp.sum(came * came, axis=1, keepdims=True)
        line = jnp.sum(jnp.where(r1 % count == r0, squares, 0.0), axis=0, keepdims=True)
        qsend[ch] = line
        qrecv[32 * ch + me_tp] = line
        gained = came * gain
        first = (r0 // 2) % 2 == 0
        return jnp.where(first, gained, 0.0).astype(BF), jnp.where(first, 0.0, gained).astype(BF)

    def squares_told(ch):
        for to in far_tp:
            send(qsend.at[ch], qrecv.at[32 * ch + me_tp], q_s, q_r.at[ch], tp=to).start()

    def small_multiplied(ch):
        e0, e1 = rows_split(ch, 8 * ch, 8)
        squares_told(ch)
        for half in range(2):
            for s in range(2):
                at = 64 * half + 32 * s
                xsm[ch, half, at : at + 32, 256 * s : 256 * s + 128] = e0
                xsm[ch, half, at : at + 32, 256 * s + 128 : 256 * s + 256] = e1
        for some in STAGES:
            low = jnp.concatenate([wt[ys[dy], 0:64, :] for dy in some], axis=0)
            high = jnp.concatenate([wt[ys[dy], 64:128, :] for dy in some], axis=0)
            part = dot(low, xsm[ch, 0], NT) + dot(high, xsm[ch, 1], NT)
            for k, dy in enumerate(some):
                for xp in range(NX):
                    at = 64 * k + 16 * xp
                    bsend[32 * ch + ys[dy] * NX + xp] = part[at : at + 16, :].astype(BF)
            for dy in some:
                for dx in FAR_X:
                    if dy or dx:
                        to = ys[dy] * NX + xs[dx]
                        send(bsend.at[32 * ch + to], brecv.at[32 * ch + me_tp], b_s, b_r.at[ch], tp=to).start()
        brecv[32 * ch + me_tp] = bsend[32 * ch + me_tp]

    def scale_of(ch):
        wait_bytes(qrecv.at[pl.ds(0, 31)], q_r.at[ch])
        return lax.rsqrt(jnp.sum(qrecv[32 * ch : 32 * ch + 32], axis=0) / D + EPS)

    def units_told(ch, units):
        hid[32 * ch + me_tp] = units.astype(BF)
        for to in far_tp:
            send(hid.at[32 * ch + me_tp], hid.at[32 * ch + me_tp], c_s, c_r.at[ch], tp=to).start()

    def small_summed(ch):
        wait_bytes(brecv.at[pl.ds(0, 31)], b_r.at[ch])
        total = jnp.sum(brecv[32 * ch : 32 * ch + 32].astype(F32), axis=0)
        v = total * scale_of(ch)
        units_told(ch, silu(v) * pltpu.roll(v, 96, 1))

    def large_multiplied():
        e0, e1 = rows_split(2, 16, 16)
        for s in range(2):
            xbd[64 * s : 64 * s + 64, 256 * s : 256 * s + 128] = e0
            xbd[64 * s : 64 * s + 64, 256 * s + 128 : 256 * s + 256] = e1
        for some in (FAR_Y[:4], FAR_Y[4:]):
            part = dot(jnp.concatenate([wt[ys[dy]] for dy in some], axis=0), xbd[...], NT)
            for k, dy in enumerate(some):
                for xp in range(NX):
                    at = 128 * k + 16 * xp
                    xsend[ys[dy] * NX + xp, 0:16, :] = part[at : at + 16, :].astype(BF)
                    xsend[ys[dy] * NX + xp, 16:32, :] = part[at + 64 : at + 80, :].astype(BF)
            for dy in some:
                yp = ys[dy]
                for dx in (2, 1, 3):
                    xp = xs[dx]
                    send(
                        xsend.at[yp * NX + xp], xrecv.at[yp * NX + x], bx_s, bx_r.at[FAR_Y.index(dy) // 4], tp=y * NX + xp
                    ).start()
        squares_told(2)

    def large_summed_over_x():
        total = None
        for at, dy in enumerate(FAR_Y):
            yp = ys[dy]
            if at % 4 == 0:
                wait_bytes(xrecv.at[pl.ds(0, 12)], bx_r.at[at // 4])
            acc = xsend[yp * NX + x].astype(F32)
            for dx in (1, 3, 2):
                acc = acc + xrecv[yp * NX + xs[dx]].astype(F32)
            if dy == 0:
                total = acc
            else:
                ysend[yp] = acc.astype(BF)
                send(ysend.at[yp], yrecv.at[y], by_s, by_r, tp=yp * NX + x).start()
        return total

    def large_summed_over_y(total):
        wait_bytes(yrecv.at[pl.ds(0, 7)], by_r)
        for dy in NEAR_Y[1:]:
            total = total + yrecv[ys[dy]].astype(F32)
        v = total * scale_of(2)
        h = silu(v) * pltpu.roll(v, 64, 1)
        units_told(2, jnp.where(lane < 64, h[0:16, :], pltpu.roll(h[16:32, :], 64, 1)))

    def given_back(ch, start, blocks):
        wait_bytes(hid.at[pl.ds(0, 31)], c_r.at[ch])
        both = dot(dt[...], hid[32 * ch : 32 * ch + 32].reshape(512, 128))
        even = (lax.broadcasted_iota(jnp.int32, (128, 128), 1) // 2) % 2 == 0
        low = jnp.where(even, both[0:128, :], both[128:256, :])
        high = jnp.where(even, both[256:384, :], both[384:512, :])
        rows[...] = (low + pltpu.roll(high, 64, 1)).T
        for b in range(blocks):
            dsend[start + b] = rows[4 * b : 4 * b + 4, :].astype(BF)
        for b in range(start, start + blocks):
            @pl.when(me_ep != b)
            def _():
                send(dsend.at[b], drecv.at[me_ep], d_s, d_r, ep=b).start()

    rows_came(0)
    small_multiplied(0)
    rows_came(2)
    rows_came(3)
    large_multiplied()
    rows_came(1)
    small_multiplied(1)
    small_summed(0)

    wait_bytes(srecv.at[pl.ds(0, 31)], s_r)
    shared_sum = jnp.sum(srecv[...].astype(F32), axis=0)
    own_scale = lax.rsqrt((shared_sum[8:9, :] + shared_sum[9:10, :]) / D + EPS)
    hsh[me_tp] = (silu(shared_sum[0:4, :] * own_scale) * (shared_sum[4:8, :] * own_scale)).astype(BF)
    for to in far_tp:
        send(hsh.at[me_tp], hsh.at[me_tp], h_s, h_r, tp=to).start()

    total2 = large_summed_over_x()
    small_summed(1)
    given_back(0, 0, 8)
    large_summed_over_y(total2)
    given_back(1, 8, 8)

    @pl.when(z // 8 == 0)
    def _():
        drecv[me_ep] = dsend[me_ep]

    @pl.when(z // 8 == 1)
    def _():
        given_back(2, 16, 16)
        drecv[me_ep] = dsend[me_ep]

    wait_bytes(hsh.at[pl.ds(0, 31)], h_r)
    for p in range(NTP):
        rows[4 * p : 4 * p + 4, :] = hsh[p].astype(F32)
    turned = rows[...].T.astype(BF)
    shared_out = jnp.zeros((16, 128), F32)
    for g in range(8):
        shared_out = shared_out + dot(turned[16 * g : 16 * g + 16, :], sd[128 * g : 128 * g + 128, :])

    wait_bytes(drecv.at[pl.ds(0, 31)], d_r)
    for b in range(NEP):
        rows[4 * b : 4 * b + 4, :] = drecv[b].astype(F32)
    given = rows[...].astype(BF)
    parts = dot(jnp.concatenate([w_hi, w_mid, w_lo], axis=0), given)
    combined = parts[0:16, :] + parts[16:32, :] + parts[32:48, :] + shared_out
    out_squares = jnp.sum(combined * combined, axis=1, keepdims=True)
    out_line = jnp.sum(jnp.where(lane == sub, out_squares, 0.0), axis=0, keepdims=True)
    esend[...] = out_line
    for to in far_tp:
        send(esend, erecv.at[me_tp], e_s, e_r, tp=to).start()
    erecv[me_tp] = out_line

    @pl.when(z // 8 == 0)
    def _():
        given_back(2, 16, 16)

    wait_bytes(erecv.at[pl.ds(0, 31)], e_r)
    all_squares = jnp.sum(erecv[...], axis=0)
    column = jnp.sum(jnp.where(lane == sub, all_squares, 0.0), axis=1, keepdims=True)
    out_scale = lax.rsqrt(column / D + EPS)
    out_ref[...] = (combined * out_scale * og[...].astype(F32)).astype(BF)

    for ref, sem in (
        (asend.at[pl.ds(0, 31)], a_s), (ssend.at[pl.ds(0, 31)], s_s), (hsh.at[pl.ds(0, 31)], h_s),
        (dsend.at[pl.ds(0, 31)], d_s), (erecv.at[pl.ds(0, 31)], e_s), (bsend.at[pl.ds(0, 62)], b_s),
        (xsend.at[pl.ds(0, 24)], bx_s), (ysend.at[pl.ds(0, 7)], by_s), (hid.at[pl.ds(0, 93)], c_s),
        (qrecv.at[pl.ds(0, 93)], q_s),
    ):
        wait_bytes(ref, sem)


def solution(mesh):
    def on_device(tokens, routes, gates, pre_gain, eg, eu, ed, sg, su, sd, out_gain):
        dma = pltpu.SemaphoreType.DMA
        hbm = pl.BlockSpec(memory_space=pl.ANY)
        vmem = pl.BlockSpec(memory_space=pltpu.VMEM)
        return pl.pallas_call(
            kernel,
            name="experts",
            out_shape=jax.ShapeDtypeStruct((16, 128), BF),
            in_specs=[hbm] + [vmem] * 3 + [hbm] * 6 + [vmem],
            out_specs=pl.BlockSpec(memory_space=pltpu.VMEM),
            scratch_shapes=[
                pltpu.VMEM((16, 128), BF), pltpu.VMEM((2, 128, 1024), BF), pltpu.VMEM((2, 128, 1024), BF),
                pltpu.VMEM((2, 1024, 128), BF), pltpu.VMEM((128, 1024), BF), pltpu.VMEM((128, 1024), BF),
                pltpu.VMEM((1024, 128), BF),
                pltpu.VMEM((8, 128, 512), BF), pltpu.VMEM((256, 1024), BF), pltpu.VMEM((512, 512), BF),
                pltpu.VMEM((32, 4, 128), BF), pltpu.VMEM((32, 4, 128), BF), pltpu.VMEM((128, 128), F32),
                pltpu.VMEM((2, 2, 128, 512), BF), pltpu.VMEM((128, 512), BF), pltpu.VMEM((128, 1024), BF),
                pltpu.VMEM((32, 16, 128), BF), pltpu.VMEM((32, 16, 128), BF), pltpu.VMEM((32, 4, 128), BF),
                pltpu.VMEM((64, 16, 128), BF), pltpu.VMEM((64, 16, 128), BF),
                pltpu.VMEM((32, 32, 128), BF), pltpu.VMEM((32, 32, 128), BF),
                pltpu.VMEM((8, 32, 128), BF), pltpu.VMEM((8, 32, 128), BF),
                pltpu.VMEM((3, 1, 128), F32), pltpu.VMEM((96, 1, 128), F32),
                pltpu.VMEM((96, 16, 128), BF),
                pltpu.VMEM((32, 4, 128), BF), pltpu.VMEM((32, 4, 128), BF),
                pltpu.VMEM((1, 128), F32), pltpu.VMEM((32, 1, 128), F32),
                dma((7,)), dma, dma((4,)), dma, dma, dma, dma, dma, dma((2,)), dma, dma((2,)), dma, dma,
                dma, dma((3,)), dma, dma((3,)), dma, dma, dma, dma,
            ],
            compiler_params=pltpu.CompilerParams(collective_id=0, has_side_effects=True, vmem_limit_bytes=55212 * 1024),
        )(tokens, routes.T, gates.T, pre_gain.reshape(1, 128), eg, eu, ed, sg, su, sd, out_gain.reshape(1, 128))

    return jax.shard_map(
        on_device,
        mesh=mesh,
        in_specs=(
            P("ep", "tp"), P("ep", None), P("ep", None), P("tp"), P("ep", "tp", None), P("ep", "tp", None),
            P("ep", None, "tp"), P("tp", None), P("tp", None), P(None, "tp"), P("tp"),
        ),
        out_specs=P("ep", "tp"),
        check_vma=False,
    )
```
